32 devices in a mesh: gr: 2 (over x), fs: 8 (over z, y), tp: 2 (over core).
Axes of the slice: x: 2, y: 2, z: 4, core: 2. Of those that a mesh axis runs over, the one named last changes fastest.
Arguments:
- prompt: bfloat16 [3072, 2048], P(('gr', 'fs', 'tp')), may hold values from -6 to 6
- norm_first: float32 [2048], P(('gr', 'fs')), may hold values from 0.1 to 1.9
- gate_first: float32 [2048, 5632], P(('gr', 'fs'), 'tp'), may hold values from -6 to 6
- up_first: float32 [2048, 5632], P(('gr', 'fs'), 'tp'), may hold values from -6 to 6
- down_first: float32 [2048, 5632], P(('gr', 'fs'), 'tp'), may hold values from -6 to 6
- norm_second: float32 [2048], P(('gr', 'fs')), may hold values from 0.1 to 1.9
- gate_second: float32 [2048, 5632], P(('gr', 'fs'), 'tp'), may hold values from -6 to 6
- up_second: float32 [2048, 5632], P(('gr', 'fs'), 'tp'), may hold values from -6 to 6
- down_second: float32 [2048, 5632], P(('gr', 'fs'), 'tp'), may hold values from -6 to 6
Outputs:
- served_gate_first: bfloat16 [2048, 5632], P(None, 'fs')
- served_up_first: bfloat16 [2048, 5632], P(None, 'fs')
- served_down_first: bfloat16 [2048, 5632], P(None, 'fs')
- served_gate_second: bfloat16 [2048, 5632], P(None, 'fs')
- served_up_second: bfloat16 [2048, 5632], P(None, 'fs')
- served_down_second: bfloat16 [2048, 5632], P(None, 'fs')
- result: bfloat16 [3072, 2048], P(('gr', 'fs', 'tp'))
The draws below stay inside these ranges and needn't reach their ends.
All inputs are finite; a program needn't handle non-finite values.
Results may differ from the reference program's by a relative error of at most 0.015.
Values may be sent and summed in bfloat16 or wider, within the bound.
A program may use at most 128 MiB of HBM per device.

```python
import jax
import jax.numpy as jnp
from jax import lax

D = 2048
FF = 5632
FF_BLK = 704
TOKENS = 3072


def block_scale(key, shape, cuts, least, high):
    factor_of = 1.0
    for axis_at, parts in cuts:
        heights = jax.random.uniform(jax.random.fold_in(jax.random.fold_in(key, 6), axis_at), (parts,), jnp.float32, least / len(cuts), high / len(cuts))
        factor_of = factor_of * jnp.repeat(jnp.exp(heights), shape[axis_at] // parts).reshape((-1,) + (1,) * (len(shape) - 1 - axis_at))
    return factor_of


def scatter_about(stream_key, extent, spread, most, pieces=(), kind=jnp.bfloat16):
    level = block_scale(stream_key, extent, pieces, -0.22, 0.18) if pieces else 1.0
    drawn = jax.random.normal(stream_key, extent, jnp.float32) * spread * level
    return jnp.minimum(jnp.maximum(drawn, -most), most).astype(kind)


def setup_inputs(seed: int = 0) -> dict:
    seeds = jax.random.split(jax.random.key(seed), 10)
    prompt = scatter_about(seeds[0], (TOKENS, D), 1.0, 6.0, ((0, 32),))
    norm_first = jnp.clip(1.0 + 0.18 * jax.random.normal(seeds[1], (D,), jnp.float32), 0.1, 1.9)
    gate_first = scatter_about(seeds[2], (D, FF), 1.0, 6.0, ((0, 16), (1, 2)), jnp.float32)
    up_first = scatter_about(seeds[3], (D, FF), 1.0, 6.0, ((0, 16), (1, 2)), jnp.float32)
    down_first = scatter_about(seeds[4], (D, FF), 1.0, 6.0, ((0, 16), (1, 2)), jnp.float32)
    norm_second = jnp.clip(1.0 + 0.18 * jax.random.normal(seeds[5], (D,), jnp.float32), 0.1, 1.9)
    gate_second = scatter_about(seeds[6], (D, FF), 1.0, 6.0, ((0, 16), (1, 2)), jnp.float32)
    up_second = scatter_about(seeds[7], (D, FF), 1.0, 6.0, ((0, 16), (1, 2)), jnp.float32)
    down_second = scatter_about(seeds[8], (D, FF), 1.0, 6.0, ((0, 16), (1, 2)), jnp.float32)
    return dict(prompt=prompt, norm_first=norm_first, gate_first=gate_first, up_first=up_first, down_first=down_first, norm_second=norm_second, gate_second=gate_second, up_second=up_second, down_second=down_second)


EPS = 1e-06

def fold_rows(gain, weight):
    return (gain[:, None] * weight).astype(jnp.bfloat16)

def half_step(residual, gate_weight, up_weight, down_weight):
    resid_f = residual.astype(jnp.float32)
    normed = (resid_f * lax.rsqrt(lax.optimization_barrier(jnp.mean(resid_f * resid_f, axis=-1, keepdims=True)) + EPS)).astype(jnp.bfloat16)
    gate_pre = jnp.dot(normed, gate_weight, preferred_element_type=jnp.float32) * D ** (-0.5)
    up_pre = jnp.dot(normed, up_weight, preferred_element_type=jnp.float32) * D ** (-0.5)
    hidden = (jax.nn.silu(gate_pre) * up_pre).astype(jnp.bfloat16)

    def add_block(running, block_index):
        offset = block_index * FF_BLK
        hid_block = lax.dynamic_slice_in_dim(hidden, offset, FF_BLK, 1)
        down_block = lax.dynamic_slice_in_dim(down_weight, offset, FF_BLK, 1)
        partial_sum = lax.dot_general(hid_block, down_block, (((1,), (1,)), ((), ())), preferred_element_type=jnp.float32) * FF ** (-0.5)
        partial_sum = lax.optimization_barrier(partial_sum.astype(jnp.bfloat16)).astype(jnp.float32)
        return (running + partial_sum, None)
    start_sum = jnp.zeros((residual.shape[0], D), jnp.float32)
    branch, _ = lax.scan(add_block, start_sum, jnp.arange(FF // FF_BLK, dtype=jnp.int32))
    return (resid_f + 0.5 * branch).astype(jnp.bfloat16)

def reference(prompt, norm_first, gate_first, up_first, down_first, norm_second, gate_second, up_second, down_second):
    served_gate_first = fold_rows(norm_first, gate_first)
    served_up_first = fold_rows(norm_first, up_first)
    served_down_first = down_first.astype(jnp.bfloat16)
    served_gate_second = fold_rows(norm_second, gate_second)
    served_up_second = fold_rows(norm_second, up_second)
    served_down_second = down_second.astype(jnp.bfloat16)
    middle = half_step(prompt, served_gate_first, served_up_first, served_down_first)
    result = half_step(middle, served_gate_second, served_up_second, served_down_second)
    return (served_gate_first, served_up_first, served_down_first, served_gate_second, served_up_second, served_down_second, result)
```

```python
import functools

import jax
import jax.numpy as jnp
from jax import lax
from jax.experimental import pallas as pl
from jax.experimental.pallas import tpu as pltpu
from jax.sharding import PartitionSpec as P

EPS = 1e-06
MESH = pl.DeviceIdType.MESH


def fold_rows(gain, weight):
    return (gain[:, None] * weight).astype(jnp.bfloat16)


def relayout_kernel(sizes, pieces, *refs):
    gr, fs, tp = sizes
    mats, blocks, rows, _ = pieces.shape
    outs = refs[:mats]
    first_send, first_recv, gr_send, gr_recv, tp_send, tp_recv = refs[mats:]
    g, f, t = lax.axis_index("gr"), lax.axis_index("fs"), lax.axis_index("tp")
    sub = rows // tp

    def rows_of(m, from_gr, from_fs, core):
        start = pl.multiple_of((from_gr * fs + from_fs) * rows + core * sub, sub)
        return outs[m].at[pl.ds(start, sub)]

    def remote(src, dst, send_sem, recv_sem, device):
        return pltpu.make_async_remote_copy(
            src_ref=src,
            dst_ref=dst,
            send_sem=send_sem,
            recv_sem=recv_sem,
            device_id=device,
            device_id_type=MESH,
        )

    def first_copies(step, act):
        slot = (step + f) % blocks
        block = t * blocks + slot
        for core in range(tp):
            mine = jnp.logical_and(block == f, t == core)
            for m in range(mats):
                source = pieces.at[m, slot, pl.ds(core * sub, sub)]
                target = rows_of(m, g, f, core)
                act(
                    mine,
                    lambda: pltpu.make_async_copy(source, target, first_recv.at[m, f]),
                    lambda: remote(
                        source,
                        target,
                        first_send.at[m, slot, core],
                        first_recv.at[m, f],
                        (g, block, core),
                    ),
                )

    def start(mine, local, far):
        @pl.when(mine)
        def _():
            local().start()

        @pl.when(jnp.logical_not(mine))
        def _():
            far().start()

    def finish(mine, local, far):
        @pl.when(jnp.logical_not(mine))
        def _():
            far().wait_send()

    def origin(step):
        return ((f // blocks + step % tp) % tp) * blocks + (f + blocks - step // tp) % blocks

    def to_peers(m, ref):
        for hop in range(1, tp):
            remote(ref, ref, tp_send.at[m], tp_recv.at[m], (g, f, (t + hop) % tp)).start()

    def send_first(step, carry):
        first_copies(step, start)
        return carry

    def pass_on(step, carry):
        source = origin(step)
        for m in range(mats):
            ref = rows_of(m, g, source, t)
            pltpu.make_async_copy(ref, ref, first_recv.at[m, source]).wait()
            for hop in range(1, gr):
                remote(
                    ref,
                    ref,
                    gr_send.at[m],
                    gr_recv.at[m, hop - 1, source],
                    ((g + hop) % gr, f, t),
                ).start()
            to_peers(m, ref)
        return carry

    def pass_on_far(step, carry):
        source = origin(step)
        for m in range(mats):
            for hop in range(1, gr):
                ref = rows_of(m, (g + gr - hop) % gr, source, t)
                pltpu.make_async_copy(ref, ref, gr_recv.at[m, hop - 1, source]).wait()
                to_peers(m, ref)
        return carry

    def finish_first(step, carry):
        first_copies(step, finish)
        return carry

    lax.fori_loop(0, blocks, send_first, 0)
    lax.fori_loop(0, fs, pass_on, 0)
    lax.fori_loop(0, fs, pass_on_far, 0)
    lax.fori_loop(0, blocks, finish_first, 0)

    def wait_rows(m, count, sem):
        if count:
            ref = outs[m].at[pl.ds(0, count)]
            pltpu.make_async_copy(ref, ref, sem).wait()

    for m in range(mats):
        wait_rows(m, fs * sub * (gr - 1), gr_send.at[m])
        wait_rows(m, gr * fs * sub * (tp - 1), tp_send.at[m])
        wait_rows(m, gr * fs * sub * (tp - 1), tp_recv.at[m])


def relayout(pieces, sizes):
    gr, fs, tp = sizes
    mats, blocks, rows, width = pieces.shape
    total = gr * fs * rows
    served = jax.ShapeDtypeStruct((total, width), pieces.dtype)
    return pl.pallas_call(
        functools.partial(relayout_kernel, sizes),
        out_shape=[served] * mats,
        in_specs=[pl.BlockSpec(memory_space=pltpu.VMEM)],
        out_specs=[pl.BlockSpec(memory_space=pl.ANY)] * mats,
        scratch_shapes=[
            pltpu.SemaphoreType.DMA((mats, blocks, tp)),
            pltpu.SemaphoreType.DMA((mats, fs)),
            pltpu.SemaphoreType.DMA((mats,)),
            pltpu.SemaphoreType.DMA((mats, max(gr - 1, 1), fs)),
            pltpu.SemaphoreType.DMA((mats,)),
            pltpu.SemaphoreType.DMA((mats,)),
        ],
        compiler_params=pltpu.CompilerParams(has_side_effects=True),
        cost_estimate=pl.CostEstimate(
            flops=0, bytes_accessed=mats * total * width * 24, transcendentals=0
        ),
        name="relayout",
    )(pieces)


def cut(matrices, blocks):
    rows, columns = matrices[0].shape
    return jnp.stack(
        [m.reshape(rows, blocks, columns // blocks).transpose(1, 0, 2) for m in matrices]
    )


def normed_tokens(resid_f):
    return (
        resid_f * lax.rsqrt(jnp.mean(resid_f * resid_f, axis=-1, keepdims=True) + EPS)
    ).astype(jnp.bfloat16)


def partial_branch(tokens_in, weights):
    gate_weight, up_weight, down_weight = weights
    in_scale = gate_weight.shape[0] ** (-0.5)
    out_scale = (down_weight.shape[1] * lax.axis_size("fs")) ** (-0.5)
    gate_pre = jnp.dot(tokens_in, gate_weight, preferred_element_type=jnp.float32) * in_scale
    up_pre = jnp.dot(tokens_in, up_weight, preferred_element_type=jnp.float32) * in_scale
    hidden = (jax.nn.silu(gate_pre) * up_pre).astype(jnp.bfloat16)
    return (
        lax.dot_general(
            hidden, down_weight, (((1,), (1,)), ((), ())), preferred_element_type=jnp.float32
        )
        * out_scale
    ).astype(jnp.bfloat16)


def gather_tokens(normed):
    return lax.all_gather(normed, "fs", axis=0, tiled=True)


def scatter_sum(partial):
    return lax.psum_scatter(partial, "fs", scatter_dimension=0, tiled=True)


def on_device(
    prompt,
    norm_first,
    gate_first,
    up_first,
    down_first,
    norm_second,
    gate_second,
    up_second,
    down_second,
):
    sizes = tuple(lax.axis_size(axis) for axis in ("gr", "fs", "tp"))
    blocks = sizes[1] // sizes[2]
    prompt_f = prompt.astype(jnp.float32)
    tokens_first = gather_tokens(normed_tokens(prompt_f))
    pieces_first = cut(
        [
            fold_rows(norm_first, gate_first),
            fold_rows(norm_first, up_first),
            down_first.astype(jnp.bfloat16),
        ],
        blocks,
    )
    pieces_second = cut(
        [
            fold_rows(norm_second, gate_second),
            fold_rows(norm_second, up_second),
            down_second.astype(jnp.bfloat16),
        ],
        blocks,
    )
    served_first = relayout(pieces_first, sizes)
    partial_first = partial_branch(tokens_first, served_first)
    pieces_second, partial_first = lax.optimization_barrier((pieces_second, partial_first))
    served_second = relayout(pieces_second, sizes)
    branch_first = scatter_sum(partial_first).astype(jnp.float32)
    middle = (prompt_f + 0.5 * branch_first).astype(jnp.bfloat16)
    middle_f = middle.astype(jnp.float32)
    tokens_second = gather_tokens(normed_tokens(middle_f))
    branch_second = scatter_sum(partial_branch(tokens_second, served_second)).astype(jnp.float32)
    result = (middle_f + 0.5 * branch_second).astype(jnp.bfloat16)
    return (*served_first, *served_second, result)


def solution(mesh):
    in_specs = (
        P(("gr", "fs", "tp"), None),
        P(("gr", "fs")),
        P(("gr", "fs"), "tp"),
        P(("gr", "fs"), "tp"),
        P(("gr", "fs"), "tp"),
        P(("gr", "fs")),
        P(("gr", "fs"), "tp"),
        P(("gr", "fs"), "tp"),
        P(("gr", "fs"), "tp"),
    )
    out_specs = (
        P(None, "fs"),
        P(None, "fs"),
        P(None, "fs"),
        P(None, "fs"),
        P(None, "fs"),
        P(None, "fs"),
        P(("gr", "fs", "tp"), None),
    )
    return jax.shard_map(
        on_device, mesh=mesh, in_specs=in_specs, out_specs=out_specs, check_vma=False
    )
```
